32 devices in a mesh: rep: 2 (over x), fs: 8 (over z, y), tp: 2 (over core).
Axes of the slice: x: 2, y: 2, z: 4, core: 2. Of those that a mesh axis runs over, the one named last changes fastest.
Arguments:
- tokens: bfloat16 [8192, 2048], P(('rep', 'fs'), 'tp'), may hold values from -6 to 6
- mix_gain: float32 [2048], replicated, may hold values from 0.1 to 1.9
- lru_input: float32 [2048, 2048], P('fs', 'tp'), may hold values from -0.125 to 0.125
- lru_gate: float32 [2048, 2048], P('fs', 'tp'), may hold values from -0.125 to 0.125
- lru_input_scale: float32 [2048], P('tp'), may hold values from 0.5 to 2
- lru_gate_scale: float32 [2048], P('tp'), may hold values from 0.5 to 2
- conv_weight: float32 [4, 2048], P(None, 'tp'), may hold values from -3 to 3
- recur_gate: float32 [32, 64, 64], P('tp'), may hold values from -0.75 to 0.75
- input_gate: float32 [32, 64, 64], P('tp'), may hold values from -0.75 to 0.75
- decay_rate: float32 [2048], P('tp'), may hold values from 3.5 to 9
- extra_decay: float32 [8192], P(('rep', 'fs')), may hold values from 0.0003 to 2.1
- lru_output: float32 [2048, 2048], P('tp', 'fs'), may hold values from -0.125 to 0.125
- lru_output_scale: float32 [2048], replicated, may hold values from 0.5 to 2
- ffn_gain: float32 [2048], replicated, may hold values from 0.1 to 1.9
- ffn_gate: float32 [2048, 2816], P('fs', 'tp'), may hold values from -0.125 to 0.125
- ffn_up: float32 [2048, 2816], P('fs', 'tp'), may hold values from -0.125 to 0.125
- ffn_gate_scale: float32 [2816], P('tp'), may hold values from 0.5 to 2
- ffn_up_scale: float32 [2816], P('tp'), may hold values from 0.5 to 2
- ffn_down: float32 [2816, 2048], P('tp', 'fs'), may hold values from -0.109375 to 0.109375
- ffn_down_scale: float32 [2048], replicated, may hold values from 0.5 to 2
Outputs:
- layer_out: bfloat16 [8192, 2048], P(('rep', 'fs'), 'tp')
The draws below stay inside these ranges and needn't reach their ends.
All inputs are finite; a program needn't handle non-finite values.
Results may differ from the reference program's by a relative error of at most 0.02.
Values may be sent and summed in bfloat16 or wider, within the bound.
A program may use at most 192 MiB of HBM per device.

```python
import math
import jax
import jax.numpy as jnp
from jax import lax

D = 2048
FF = 2816
BDIM = 64
LRU_BLOCKS = 32
CONV = 4
TOK_DEV = 512
LRU = 2048
SEQS = 16
TOKENS = 8192
N_TP = 2


def draw_decay_rate(key, part):
    first, second, third = jax.random.split(jax.random.fold_in(key, 11), 3)
    share = 0.5
    slow = jax.random.uniform(first, (LRU,), jnp.float32) < share
    slow_value = jax.random.uniform(second, (LRU,), jnp.float32, 8.0, 9.0)
    fast_value = jax.random.uniform(third, (LRU,), jnp.float32, 3.5, 4.5)
    return jnp.where(slow, slow_value, fast_value)


def draw_extra_decay(key, part):
    first, second, third = jax.random.split(jax.random.fold_in(key, 23), 3)
    base = jnp.exp(jax.random.uniform(first, (SEQS, 1), jnp.float32, jnp.log(0.0003), jnp.log(0.0009)))
    spots = jax.random.randint(second, (SEQS, 3), 0, TOK_DEV)
    where = jnp.arange(TOK_DEV, dtype=jnp.int32)
    hits = jnp.sum((where[None, None, :] == spots[:, :, None]).astype(jnp.float32), axis=1)
    sizes = jax.random.uniform(third, (SEQS, TOK_DEV), jnp.float32, 0.22, 0.69)
    return (base + hits * sizes).reshape(TOKENS)


def block_scale(rng, shape, cuts, smallest, top_value):
    def one(position, shards_of):
        draws = jax.random.uniform(jax.random.fold_in(jax.random.fold_in(rng, 6), position), (shards_of,), jnp.float32, smallest / len(cuts), top_value / len(cuts))
        return jnp.repeat(jnp.exp(draws), shape[position] // shards_of).reshape((-1,) + (1,) * (len(shape) - position - 1))

    loudness = one(*cuts[0])
    for cut in cuts[1:]:
        loudness = loudness * one(*cut)
    return loudness


def gaussian(rng, shape, scale, most, cuts=(), kind=jnp.bfloat16):
    entries = jax.random.normal(rng, shape, jnp.float32) * scale
    if len(cuts) > 0:
        entries = block_scale(rng, shape, cuts, -0.22, 0.18) * entries
    return jnp.clip(entries, min=-most, max=most).astype(kind)


def setup_inputs(seed: int = 0) -> dict:
    key_of = jax.random.split(jax.random.key(seed), 21)
    tokens = gaussian(key_of[0], (TOKENS, D), 1.0, 6.0, ((0, 16), (1, 2)))
    mix_gain = jnp.clip(1.0 + 0.18 * jax.random.normal(key_of[1], (D,), jnp.float32), 0.1, 1.9)
    lru_input = gaussian(key_of[2], (D, LRU), D ** -0.5, 0.125, ((0, 8), (1, 2)), jnp.float32)
    lru_gate = gaussian(key_of[3], (D, LRU), D ** -0.5, 0.125, ((0, 8), (1, 2)), jnp.float32)
    lru_input_scale = jnp.clip(jnp.exp(math.log(2.0) - 1.3862944 * jax.random.uniform(key_of[4], (LRU,), jnp.float32) ** block_scale(key_of[4], (LRU,), ((0, 2),), -0.2, 0.2)), 0.5, 2.0)
    lru_gate_scale = jnp.clip(jnp.exp(math.log(2.0) - 1.3862944 * jax.random.uniform(key_of[5], (LRU,), jnp.float32) ** block_scale(key_of[5], (LRU,), ((0, 2),), -0.2, 0.2)), 0.5, 2.0)
    conv_weight = gaussian(key_of[6], (CONV, LRU), 0.5, 3.0, ((1, 2),), jnp.float32)
    recur_gate = gaussian(key_of[7], (LRU_BLOCKS, BDIM, BDIM), BDIM ** -0.5, 0.75, ((0, 2),), jnp.float32)
    input_gate = gaussian(key_of[8], (LRU_BLOCKS, BDIM, BDIM), BDIM ** -0.5, 0.75, ((0, 2),), jnp.float32)
    decay_rate = draw_decay_rate(jax.random.fold_in(key_of[20], 71), 0)
    extra_decay = draw_extra_decay(jax.random.fold_in(key_of[20], 71), 0)
    lru_output = gaussian(key_of[11], (LRU, D), LRU ** -0.5, 0.125, ((0, 2), (1, 8)), jnp.float32)
    lru_output_scale = jnp.clip(jnp.exp(jax.random.uniform(key_of[12], (D,), jnp.float32, math.log(0.5), math.log(2.0))), 0.5, 2.0)
    ffn_gain = jnp.clip(1.0 + 0.18 * jax.random.normal(key_of[13], (D,), jnp.float32), 0.1, 1.9)
    ffn_gate = gaussian(key_of[14], (D, FF), D ** -0.5, 0.125, ((0, 8), (1, 2)), jnp.float32)
    ffn_up = gaussian(key_of[15], (D, FF), D ** -0.5, 0.125, ((0, 8), (1, 2)), jnp.float32)
    ffn_gate_scale = jnp.clip(jnp.exp(math.log(2.0) - 1.3862944 * jax.random.uniform(key_of[16], (FF,), jnp.float32) ** block_scale(key_of[16], (FF,), ((0, 2),), -0.2, 0.2)), 0.5, 2.0)
    ffn_up_scale = jnp.clip(jnp.exp(math.log(2.0) - 1.3862944 * jax.random.uniform(key_of[17], (FF,), jnp.float32) ** block_scale(key_of[17], (FF,), ((0, 2),), -0.2, 0.2)), 0.5, 2.0)
    ffn_down = gaussian(key_of[18], (FF, D), FF ** -0.5, 0.109375, ((0, 2), (1, 8)), jnp.float32)
    ffn_down_scale = jnp.clip(jnp.exp(jax.random.uniform(key_of[19], (D,), jnp.float32, math.log(0.5), math.log(2.0))), 0.5, 2.0)
    return dict(tokens=tokens, mix_gain=mix_gain, lru_input=lru_input, lru_gate=lru_gate, lru_input_scale=lru_input_scale, lru_gate_scale=lru_gate_scale, conv_weight=conv_weight, recur_gate=recur_gate, input_gate=input_gate, decay_rate=decay_rate, extra_decay=extra_decay, lru_output=lru_output, lru_output_scale=lru_output_scale, ffn_gain=ffn_gain, ffn_gate=ffn_gate, ffn_up=ffn_up, ffn_gate_scale=ffn_gate_scale, ffn_up_scale=ffn_up_scale, ffn_down=ffn_down, ffn_down_scale=ffn_down_scale)


EPS = 1e-06
RATE = 8.0

def rms_rows(rows, gain):
    values = rows.astype(jnp.float32)
    scale = lax.rsqrt(lax.optimization_barrier(jnp.mean(values * values, axis=-1, keepdims=True)) + EPS)
    return (values * scale * gain).astype(jnp.bfloat16)

def block_sum(acts, weight, blocks):
    width = acts.shape[1] // blocks
    total = jnp.zeros((acts.shape[0], weight.shape[1]), jnp.float32)
    for block in range(blocks):
        part = jnp.dot(acts[:, block * width:(block + 1) * width], weight[block * width:(block + 1) * width].astype(jnp.bfloat16), preferred_element_type=jnp.float32).astype(jnp.bfloat16)
        part = lax.optimization_barrier(part)
        total = total + part.astype(jnp.float32)
    return total

def combine(left, right):
    return (left[0] * right[0], right[0] * left[1] + right[1])

def recurrence(branch_in, branch_gate, conv_weight, recur_gate, input_gate, decay_rate, extra):
    length = branch_in.shape[0]
    taps = conv_weight.shape[0]
    values = branch_in.astype(jnp.float32)
    padded = jnp.pad(values, ((taps - 1, 0), (0, 0)))
    conv = jnp.zeros_like(values)
    for tap in range(taps):
        conv = conv + conv_weight[tap] * padded[tap:tap + length]
    nblocks, bdim = (recur_gate.shape[0], recur_gate.shape[1])
    grouped = conv.reshape(length, nblocks, bdim)
    recur = jax.nn.sigmoid(jnp.einsum('sni,nij->snj', grouped, recur_gate, precision=lax.Precision.HIGHEST).reshape(length, -1))
    ingate = jax.nn.sigmoid(jnp.einsum('sni,nij->snj', grouped, input_gate, precision=lax.Precision.HIGHEST).reshape(length, -1))
    log_rate = -RATE * jax.nn.softplus(-decay_rate) * recur - extra[:, None]
    factor = jnp.exp(log_rate)
    drive = jnp.sqrt(-jnp.expm1(2.0 * log_rate)) * (ingate * conv)
    state = lax.associative_scan(combine, (factor, drive), axis=0)[1]
    gelu_gate = jax.nn.gelu(branch_gate.astype(jnp.float32), approximate=True)
    return (state * gelu_gate).astype(jnp.bfloat16)

def reference(tokens, mix_gain, lru_input, lru_gate, lru_input_scale, lru_gate_scale, conv_weight, recur_gate, input_gate, decay_rate, extra_decay, lru_output, lru_output_scale, ffn_gain, ffn_gate, ffn_up, ffn_gate_scale, ffn_up_scale, ffn_down, ffn_down_scale):
    normed = rms_rows(tokens, mix_gain)
    branch_in = (jnp.dot(normed, lru_input.astype(jnp.bfloat16), preferred_element_type=jnp.float32) * lru_input_scale).astype(jnp.bfloat16)
    branch_gate = (jnp.dot(normed, lru_gate.astype(jnp.bfloat16), preferred_element_type=jnp.float32) * lru_gate_scale).astype(jnp.bfloat16)
    width = branch_in.shape[1]
    gated = jax.vmap(recurrence, in_axes=(0, 0, None, None, None, None, 0))(branch_in.reshape(SEQS, TOK_DEV, width), branch_gate.reshape(SEQS, TOK_DEV, width), conv_weight, recur_gate, input_gate, decay_rate, extra_decay.reshape(SEQS, TOK_DEV))
    gated = gated.reshape(TOKENS, width)
    mixed = (tokens.astype(jnp.float32) + block_sum(gated, lru_output, N_TP) * lru_output_scale).astype(jnp.bfloat16)
    normed2 = rms_rows(mixed, ffn_gain)
    gate_pre = jnp.dot(normed2, ffn_gate.astype(jnp.bfloat16), preferred_element_type=jnp.float32) * ffn_gate_scale
    up_pre = jnp.dot(normed2, ffn_up.astype(jnp.bfloat16), preferred_element_type=jnp.float32) * ffn_up_scale
    hidden = (jax.nn.silu(gate_pre) * up_pre).astype(jnp.bfloat16)
    total = block_sum(hidden, ffn_down, N_TP)
    return (mixed.astype(jnp.float32) + total * ffn_down_scale).astype(jnp.bfloat16)
```

```python
import functools

import jax
import jax.numpy as jnp
from jax import lax
from jax.experimental import pallas as pl
from jax.experimental.pallas import tpu as pltpu
from jax.sharding import PartitionSpec as P

EPS = 1e-06
RATE = 8.0
LANES = 128
FIRST = 6.0
RATE_BOTH = 23300.0
HOP = 22.5
DOT = (1.5, 0.0, 2.2)
MESH = pl.DeviceIdType.MESH


def scoped(name):
    def wrap(f):
        def inner(*args):
            with jax.named_scope(name + "".join(f"_{a}" for a in args if isinstance(a, int))):
                return f(*args)

        return inner

    return wrap


def sigmoid(v):
    return 1.0 / (1.0 + jnp.exp(-v))


def rec_block(values, gate, taps, maps, rate, extra):
    length = values.shape[0]
    ntaps = taps.shape[0]
    row = lax.broadcasted_iota(jnp.int32, values.shape, 0)
    conv = taps[ntaps - 1 : ntaps, :] * values
    for back in range(1, ntaps):
        moved = jnp.where(row >= back, pltpu.roll(values, back, 0), 0.0)
        conv = conv + taps[ntaps - 1 - back : ntaps - back, :] * moved
    mapped = jnp.dot(
        conv, maps, preferred_element_type=jnp.float32, precision=lax.Precision.HIGHEST
    )
    recur = sigmoid(mapped[:, :LANES])
    ingate = sigmoid(mapped[:, LANES:])
    log_rate = rate * recur - extra
    a = jnp.exp(log_rate)
    u = -2.0 * log_rate
    series = u * (1 - u / 2 * (1 - u / 3 * (1 - u / 4 * (1 - u / 5 * (1 - u / 6)))))
    b = jnp.sqrt(jnp.where(u < 0.25, series, 1.0 - jnp.exp(-u))) * (ingate * conv)
    inner = row % 8
    for s in (1, 2, 4):
        keep = inner >= s
        b = jnp.where(keep, a * pltpu.roll(b, s, 0) + b, b)
        a = jnp.where(keep, a * pltpu.roll(a, s, 0), a)
    groups = length // 8
    last_a = a.reshape(groups, 8, LANES)
    last_b = b.reshape(groups, 8, LANES)
    ca = jnp.broadcast_to(last_a[:, 7:8, :], last_a.shape).reshape(length, LANES)
    cb = jnp.broadcast_to(last_b[:, 7:8, :], last_b.shape).reshape(length, LANES)
    s = 8
    while s < length:
        cb_new = ca[s:] * cb[:-s] + cb[s:]
        ca_new = ca[s:] * ca[:-s]
        cb = jnp.concatenate([cb[:s], cb_new], axis=0)
        ca = jnp.concatenate([ca[:s], ca_new], axis=0)
        s *= 2
    state = jnp.concatenate([b[:8], a[8:] * cb[:-8] + b[8:]], axis=0)
    gelu = 0.5 * gate * (1.0 + jnp.tanh(0.7978845608028654 * (gate + 0.044715 * gate * gate * gate)))
    return (state * gelu).astype(jnp.bfloat16)


def layer_kernel(
    ny,
    nz,
    tokens,
    lru_input,
    lru_gate,
    lru_output,
    ffn_gate,
    ffn_up,
    ffn_down,
    extra_ref,
    mgain_ref,
    fgain_ref,
    iscale_ref,
    gscale_ref,
    oscale_ref,
    fscale_ref,
    dscale_ref,
    taps_ref,
    rmap_ref,
    imap_ref,
    decay_ref,
    o_ref,
    tok,
    ex,
    nrm,
    b0,
    b1,
    b2,
    b3,
    st_mix,
    st_out,
    st_down,
    acc,
    gated,
    hid,
    part,
    thr_s,
    thr_r,
    xs,
    xr,
    maps,
    rates,
    guscale,
    lsem,
    us,
    ur,
    ds,
    dr,
    ys,
    yr,
    ts,
    tr,
    ps,
    pr,
    xss,
    xrs,
    ms,
    mr,
):
    f32, bf16 = jnp.float32, jnp.bfloat16
    fs = ny * nz
    length, columns = tokens.shape
    c = lru_input.shape[0]
    hb = columns // c
    width = gated.shape[2]
    hidden = hid.shape[2]
    rep, tp, me = lax.axis_index("rep"), lax.axis_index("tp"), lax.axis_index("fs")
    z, y = me // ny, me % ny
    buf = (b0, b1, b2, b3)
    over_x = {"rep": 1 - rep}
    over_tp = {"tp": 1 - tp}
    over_y = {"fs": z * ny + (1 - y)}
    half = nz // 2
    plan = (
        ((96, False), (112, False), (48, True)),
        ((416, False), (96, True)),
        ((96, False), (96, False), (64, True)),
        ((704, False),),
    )
    groups = []
    for b, parts in enumerate(plan):
        row, rows = 0, buf[b].shape[1]
        whole_rows = sum(n for n, _ in parts)
        for i, (n, both) in enumerate(parts):
            n = rows - row if i + 1 == len(parts) else max(16, n * rows // whole_rows // 16 * 16)
            groups.append((b, row, n, both and ny > 1))
            row += n

    clock = [0.0]
    eta, slots, at_time = {}, [], FIRST
    for g, (b, _, n, both) in enumerate(groups):
        size = n * buf[b].shape[2] * (2 if both else 1)
        for k in range(1, nz):
            at_time += size / RATE_BOTH
            eta[g, k] = at_time
            slots.append((g, k))

    def copy(src, dst, s, r, where):
        return pltpu.make_async_remote_copy(
            src_ref=src, dst_ref=dst, send_sem=s, recv_sem=r, device_id=where, device_id_type=MESH
        )

    def piece(g, at, w):
        b, row, rows, _ = groups[g]
        return buf[b].at[at * ny + (y if w == 0 else 1 - y), pl.ds(row, rows)]

    def tracks(g):
        return (0, 1) if groups[g][3] else (0,)

    def up(g, w, k, at):
        p = piece(g, at, w)
        return copy(p, p, us.at[g, w, k], ur.at[g, w, k], {"fs": lax.rem(z + 1, nz) * ny + y})

    def down_z(g, w, k, at):
        p = piece(g, at, w)
        return copy(
            p, p, ds.at[g, w, k], dr.at[g, w, k], {"fs": lax.rem(z + nz - 1, nz) * ny + y}
        )

    def from_z(d):
        return lax.rem(z - d + nz, nz)

    def over(g, d, w=0):
        p = piece(g, from_z(d), w)
        return copy(p, p, ys.at[g, d], yr.at[g, d], over_y)

    def can_up(k):
        return (z + 1 < nz) & (z >= k - 1)

    def can_down(k):
        return (z > 0) & (z + k <= nz)

    def own_y(g):
        if g < len(groups) and ny > 1:
            over(g, 0).start()

    def own_z(g):
        if g < len(groups):
            if groups[g][3]:
                over(g, 0, 1).wait_recv()
            for w in tracks(g):

                @pl.when(can_up(1))
                def _():
                    up(g, w, 1, z).start()

                @pl.when(can_down(1))
                def _():
                    down_z(g, w, 1, z).start()

    @scoped("slot")
    def slot(g, k):
        if k == nz - 1:
            own_z(g + 1)
            own_y(g + 2)

        @pl.when(z >= k)
        def _():
            for w in tracks(g):
                up(g, w, k, z - k).wait_recv()
                if k + 1 < nz:

                    @pl.when(can_up(k + 1))
                    def _():
                        up(g, w, k + 1, z - k).start()

            if ny > 1 and not groups[g][3]:
                over(g, k).start()

        @pl.when(z + k < nz)
        def _():
            for w in tracks(g):
                down_z(g, w, k, z + k).wait_recv()
                if k + 1 < nz:

                    @pl.when(can_down(k + 1))
                    def _():
                        down_z(g, w, k + 1, z + k).start()

            if ny > 1 and not groups[g][3]:
                over(g, nz - k).start()

    def next_slot():
        key = slots.pop(0)
        clock[0] = max(clock[0], eta[key])
        slot(*key)

    def pump(until):
        while slots and eta[slots[0]] <= until:
            next_slot()

    def need(b, k):
        g = max(i for i, group in enumerate(groups) if group[0] == b)
        while slots and slots[0] <= (g, k):
            next_slot()

    def run(cost, f, *args):
        pump(clock[0] + cost / 2)
        f(*args)
        clock[0] += cost

    def wait_until(when, f, *args):
        pump(when)
        f(*args)
        clock[0] = max(clock[0], when)

    def nth(i):
        near = jnp.minimum(z, nz - 1 - z)
        step = i // 2 + 1
        both = z - step if i % 2 == 0 else z + step
        far = i - near + 1
        rest = jnp.where(z > nz - 1 - z, z - far, z + far)
        return jnp.where(i < 2 * near, both, rest)

    def stage(src, dst, i):
        return pltpu.make_async_copy(src, dst, lsem.at[i])

    mine_cols = pl.ds(pl.multiple_of(rep * width, LANES), width)
    loads = [
        stage(lru_input.at[:, mine_cols], st_mix.at[0], 0),
        stage(lru_gate.at[:, mine_cols], st_mix.at[1], 1),
        stage(tokens, tok.at[0, tp], 2),
        stage(lru_output.at[pl.ds(pl.multiple_of(rep * width, 8), width)], st_out, 3),
        stage(ffn_gate, acc.at[0, :c], 4),
        stage(ffn_up, acc.at[1, :c], 5),
        stage(ffn_down.at[pl.ds(pl.multiple_of(rep * hidden, 8), hidden)], st_down, 6),
    ]
    for load in loads:
        load.start()

    barrier = pltpu.get_barrier_semaphore()

    def greet(where):
        pl.semaphore_signal(barrier, inc=1, device_id=where, device_id_type=MESH)

    greet(over_x)
    greet(over_tp)
    if ny > 1:
        greet(over_y)
    pl.when(z + 1 < nz)(lambda: greet({"fs": lax.rem(z + 1, nz) * ny + y}))
    pl.when(z > 0)(lambda: greet({"fs": lax.rem(z + nz - 1, nz) * ny + y}))

    loads[0].wait()
    loads[1].wait()
    b0[me, :, :width] = st_mix[0].astype(bf16)
    b0[me, :, width:] = st_mix[1].astype(bf16)
    ex[0] = jnp.broadcast_to(extra_ref[...], ex.shape[1:])
    loads[2].wait()

    along_z = jnp.where(z > 0, 1, 0) + jnp.where(z + 1 < nz, 1, 0)
    pl.semaphore_wait(barrier, (3 if ny > 1 else 2) + along_z)

    def tok_copy(s, i, where, to):
        return copy(tok.at[s, tp], tok.at[to, tp], ts.at[i], tr.at[i], where)

    tok_tp = tok_copy(0, 0, over_tp, 0)
    tok_x = tok_copy(0, 1, over_x, 1)
    tok_xtp = tok_copy(1, 2, over_tp, 1)
    extra_x = copy(ex.at[0], ex.at[1], ts.at[3], tr.at[3], over_x)
    own_z(0)
    own_y(0)
    tok_tp.start()
    tok_x.start()
    extra_x.start()
    loads[3].wait()
    b1[me] = st_out[...].astype(bf16)
    own_y(1)

    @scoped("wait")
    def arrived(c):
        c.wait_recv()

    main = hidden // LANES * LANES
    rest = hidden - main

    @scoped("pack")
    def pack():
        loads[4].wait()
        loads[5].wait()
        step = 32

        def mine(v):
            return jnp.where(rep == 0, v, pltpu.roll(v, hidden, 1))

        def pair(g, u):
            g, u = mine(g), mine(u)
            out = [g[:, :main], u[:, :main]]
            if rest:
                g, u = g[:, main : main + LANES], u[:, main : main + LANES]
                lane = lax.broadcasted_iota(jnp.int32, g.shape, 1)
                out.append(jnp.where(lane < rest, g, pltpu.roll(u, rest, 1)))
            return out

        def body(i, _):
            r = pl.ds(pl.multiple_of(i * step, step), step)
            out = pair(acc[0, r, :], acc[1, r, :])
            b2[me, r, :main] = out[0].astype(bf16)
            b2[me, r, main : 2 * main] = out[1].astype(bf16)
            if rest:
                b2[me, r, 2 * main :] = out[2].astype(bf16)
            return 0

        lax.fori_loop(0, c // step, body, 0)
        wide = (8, 2 * hidden)
        out = pair(
            jnp.broadcast_to(fscale_ref[0:1, :], wide), jnp.broadcast_to(fscale_ref[1:2, :], wide)
        )
        guscale[:, :main] = out[0]
        guscale[:, main : 2 * main] = out[1]
        if rest:
            guscale[:, 2 * main :] = out[2]
        loads[6].wait()
        b3[me] = st_down[...].astype(bf16)

    @scoped("tables")
    def tables():
        v = -decay_ref[:, mine_cols]
        e = jnp.exp(-jnp.abs(v))
        q = e / (2.0 + e)
        p = q * q
        poly = jnp.full_like(p, 1.0 / 17)
        for odd in range(15, 0, -2):
            poly = poly * p + 1.0 / odd
        rates[...] = -RATE * (jnp.maximum(v, 0.0) + 2.0 * q * poly)
        bdim = rmap_ref.shape[1]
        per = LANES // bdim
        zero = jnp.zeros((bdim, bdim), f32)
        for i in range(width // LANES):
            for p_ in range(per):
                for k, ref in enumerate((rmap_ref, imap_ref)):
                    block = ref[rep * (width // bdim) + i * per + p_]
                    maps[i, p_ * bdim : (p_ + 1) * bdim, k * LANES : (k + 1) * LANES] = (
                        jnp.concatenate(
                            [block if q_ == p_ else zero for q_ in range(per)], axis=1
                        )
                    )

    @scoped("norm")
    def norm(read, s, gain):
        step = 128

        def body(i, _):
            r = pl.ds(pl.multiple_of(i * step, step), step)
            total = jnp.zeros((step, 1), f32)
            for b in range(fs):
                v = read(b, r).astype(f32)
                total = total + jnp.sum(v * v, axis=-1, keepdims=True)
            scale = lax.rsqrt(total / (fs * c) + EPS)
            for b in range(fs):
                v = read(b, r).astype(f32)
                nrm[s, b, r, :] = (v * scale * gain[:, b * c : (b + 1) * c]).astype(bf16)
            return 0

        lax.fori_loop(0, length // step, body, 0)

    def tok_block(s):
        return lambda b, r: tok[s, b // hb, r, b % hb * c : (b % hb + 1) * c]

    @scoped("dot")
    def dot(b, s, at, first):
        n = buf[b].shape[2]
        tile = 256
        src = pl.ds(at * ny, ny)
        rows = jnp.concatenate([nrm[s, at * ny + i] for i in range(ny)], axis=1)

        def one(cols):
            v = jnp.dot(
                rows, buf[b][src, :, cols].reshape(ny * c, -1), preferred_element_type=f32
            )
            if first:
                acc[s, :, cols] = v
            else:
                acc[s, :, cols] += v

        def body(i, _):
            one(pl.ds(pl.multiple_of(i * tile, tile), tile))
            return 0

        lax.fori_loop(0, n // tile, body, 0)
        if n % tile:
            one(pl.ds(n // tile * tile, n % tile))

    def from_y(b, d):
        if ny > 1:
            for g, group in enumerate(groups):
                if group[0] == b and not group[3]:
                    p = piece(g, lax.rem(z - d + nz, nz), 1)
                    arrived(copy(p, p, ys.at[g, d], yr.at[g, d], over_y))

    def ready(b, i):
        need(b, i + 1)
        from_y(b, 0 if i < 0 else lax.rem(z - nth(i) + nz, nz))

    def dots(b, s, i):
        run(DOT[b], dot, b, s, z if i < 0 else nth(i), i < 0)

    @scoped("recur")
    def recurrence(s, lo, hi):
        extra = jnp.transpose(ex[s])[:, :1]

        def body(i, _):
            lanes = pl.ds(pl.multiple_of(i * LANES, LANES), LANES)
            glanes = pl.ds(pl.multiple_of(width + i * LANES, LANES), LANES)
            wide = pl.ds(pl.multiple_of(rep * width + i * LANES, LANES), LANES)
            values = (acc[s, :, lanes] * iscale_ref[:, wide]).astype(bf16).astype(f32)
            gate = (acc[s, :, glanes] * gscale_ref[:, wide]).astype(bf16).astype(f32)
            gated[s, :, lanes] = rec_block(
                values, gate, taps_ref[:, wide], maps[i], rates[:, lanes], extra
            )
            return 0

        lax.fori_loop(lo, hi, body, 0)

    def tp_copy(l, s, j):
        return copy(
            thr_s.at[s, j], thr_r.at[s, j], ps.at[l, s, j], pr.at[l, s, j], over_tp
        )

    def x_copy(l, j):
        return copy(xs.at[j], xr.at[j], xss.at[l, j], xrs.at[l, j], over_x)

    @scoped("project")
    def project(l, s, j):
        acts, w = (gated, b1) if l == 0 else (hid, b3)
        theirs = jnp.dot(acts[s], w[(1 - tp) * hb + j], preferred_element_type=f32)
        thr_s[s, j] = theirs.astype(bf16)
        tp_copy(l, s, j).start()
        part[s, j] = jnp.dot(acts[s], w[tp * hb + j], preferred_element_type=f32)

    @scoped("send")
    def send_pair(l, j):
        tp_copy(l, 1, j).wait_recv()
        xs[j] = (part[1, j] + thr_r[1, j].astype(f32)).astype(bf16)
        x_copy(l, j).start()

    def own_scale(ref, j):
        return jnp.where(
            tp == 0, ref[:, j * c : (j + 1) * c], ref[:, (hb + j) * c : (hb + j + 1) * c]
        )

    chunk = max(c, LANES)
    chunks = columns // chunk

    def moved(s, to, q, i, where):
        cols = pl.ds(q * chunk, chunk)
        return copy(
            tok.at[s, tp, :, cols], tok.at[to, tp, :, cols], ms.at[i, q], mr.at[i, q], where
        )

    def m_tp(q):
        return moved(0, 0, q, 0, over_tp)

    def m_x(q):
        return moved(0, 1, q, 1, over_x)

    def m_xtp(q):
        return moved(1, 1, q, 2, over_tp)

    @scoped("mixed")
    def mixed(q):
        for j in range(q * chunk // c, (q + 1) * chunk // c):
            tp_copy(0, 0, j).wait_recv()
            x_copy(0, j).wait_recv()
            total = part[0, j] + thr_r[0, j].astype(f32) + xr[j].astype(f32)
            cols = slice(j * c, (j + 1) * c)
            tok[0, tp, :, cols] = (
                tok[0, tp, :, cols].astype(f32) + total * own_scale(oscale_ref, j)
            ).astype(bf16)
        m_x(q).start()
        m_tp(q).start()

    @scoped("hide")
    def hide(s):
        def silu_up(g, u):
            return (g / (1.0 + jnp.exp(-g)) * u).astype(bf16)

        def body(i, _):
            step = 128
            r = pl.ds(pl.multiple_of(i * step, step), step)
            for k in range(0, main, LANES):
                m = main + k
                g = acc[s, r, k : k + LANES] * guscale[0:1, k : k + LANES]
                u = acc[s, r, m : m + LANES] * guscale[0:1, m : m + LANES]
                hid[s, r, k : k + LANES] = silu_up(g, u)
            if rest:
                both = acc[s, r, 2 * main :] * guscale[0:1, 2 * main :]
                hid[s, r, main:] = silu_up(both, pltpu.roll(both, rest, 1))[:, :rest]
            return 0

        lax.fori_loop(0, length // 128, body, 0)

    def store(q):
        cols = pl.ds(q * chunk, chunk)
        return pltpu.make_async_copy(tok.at[0, tp, :, cols], o_ref.at[:, cols], lsem.at[q])

    @scoped("finish")
    def finish(q):
        m_tp(q).wait_send()
        m_x(q).wait_send()
        for j in range(q * chunk // c, (q + 1) * chunk // c):
            tp_copy(1, 0, j).wait_recv()
            x_copy(1, j).wait_recv()
            total = part[0, j] + thr_r[0, j].astype(f32) + xr[j].astype(f32)
            cols = slice(j * c, (j + 1) * c)
            tok[0, tp, :, cols] = (
                tok[0, tp, :, cols].astype(f32) + total * own_scale(dscale_ref, j)
            ).astype(bf16)
        store(q).start()

    ranks = range(-1, nz - 1)
    blocks = width // LANES
    spans = [(lo, min(lo + 2, blocks)) for lo in range(0, blocks, 2)]
    wait_until(6.0, arrived, tok_tp)
    run(1.3, norm, tok_block(0), 0, mgain_ref)
    run(1.4, pack)
    run(1.0, tables)
    ready(0, -1)
    dots(0, 0, -1)
    wait_until(27.0, arrived, tok_x)
    tok_xtp.start()
    wait_until(31.0, arrived, tok_xtp)
    run(1.3, norm, tok_block(1), 1, mgain_ref)
    for sent in (tok_tp, tok_x, tok_xtp, extra_x):
        sent.wait_send()
    dots(0, 1, -1)
    for i in ranks[1:]:
        ready(0, i)
        for s in (0, 1):
            dots(0, s, i)
    arrived(extra_x)
    for s in (1, 0):
        for span in spans:
            run(3.3, recurrence, s, *span)
    for i in ranks:
        ready(1, i)
    for j in range(hb):
        run(0.9, project, 0, 1, j)
        if j:
            run(0.3, send_pair, 0, j - 1)
    run(0.3, send_pair, 0, hb - 1)
    start = clock[0]
    for j in range(hb):
        run(0.9, project, 0, 0, j)
    hop = HOP / chunks
    for q in range(chunks):
        wait_until(start + (q + 0.8) * hop, mixed, q)
    for q in range(chunks):
        arrived(m_tp(q))
    run(1.3, norm, tok_block(0), 0, fgain_ref)
    start += (chunks + 0.2) * hop
    ready(2, -1)
    dots(2, 0, -1)
    for q in range(chunks):
        wait_until(start + (q + 1) * hop, arrived, m_x(q))
        m_xtp(q).start()
    for q in range(chunks):
        arrived(m_xtp(q))
    run(1.3, norm, tok_block(1), 1, fgain_ref)
    dots(2, 1, -1)
    for i in ranks[1:]:
        ready(2, i)
        for s in (1, 0):
            dots(2, s, i)
    run(0.8, hide, 1)
    run(0.8, hide, 0)
    for j in range(hb):
        x_copy(0, j).wait_send()
        for s in range(2):
            tp_copy(0, s, j).wait_send()

    need(3, half)
    for w in (0, 1) if ny > 1 else (0,):
        for k in range(half):
            if w:
                from_y(3, k)
                from_y(3, k + half)
            else:
                need(3, half if k == 0 else nz - 1)
            j = lax.rem(z - k + nz, half) * ny + (1 - y if w else y)
            run(0.55, project, 1, 1, j)
            run(0.55, project, 1, 0, j)
            run(0.3, send_pair, 1, j)
    for q in range(chunks):
        finish(q)

    for g, group in enumerate(groups):
        for k in range(1, nz):
            for w in tracks(g):

                @pl.when(can_up(k))
                def _():
                    up(g, w, k, z - k + 1).wait_send()

                @pl.when(can_down(k))
                def _():
                    down_z(g, w, k, z + k - 1).wait_send()

        if ny > 1:
            for d in [0] if group[3] else range(nz):
                over(g, d).wait_send()
    for j in range(hb):
        x_copy(1, j).wait_send()
        for s in range(2):
            tp_copy(1, s, j).wait_send()
    for q in range(chunks):
        m_xtp(q).wait_send()
        store(q).wait()


def layer(ny, nz, tokens, lru_input, lru_gate, lru_output, ffn_gate, ffn_up, ffn_down, *rest):
    fs = ny * nz
    length, columns = tokens.shape
    c = lru_input.shape[0]
    hb = columns // c
    width, hidden = lru_output.shape[0] // 2, ffn_down.shape[0] // 2
    bf16, f32 = jnp.bfloat16, jnp.float32
    dma = pltpu.SemaphoreType.DMA
    vmem = pl.BlockSpec(memory_space=pltpu.VMEM)
    hbm = pl.BlockSpec(memory_space=pl.ANY)
    return pl.pallas_call(
        functools.partial(layer_kernel, ny, nz),
        out_shape=jax.ShapeDtypeStruct((length, columns), bf16),
        in_specs=[hbm] * 7 + [vmem] * len(rest),
        out_specs=hbm,
        scratch_shapes=[
            pltpu.VMEM((2, 2, length, columns), bf16),
            pltpu.VMEM((2, 8, length), f32),
            pltpu.VMEM((2, fs, length, c), bf16),
            pltpu.VMEM((fs, c, 2 * width), bf16),
            pltpu.VMEM((fs, width, c), bf16),
            pltpu.VMEM((fs, c, 2 * hidden), bf16),
            pltpu.VMEM((fs, hidden, c), bf16),
            pltpu.VMEM((2, c, width), f32),
            pltpu.VMEM((width, c), f32),
            pltpu.VMEM((hidden, c), f32),
            pltpu.VMEM((2, length, 2 * max(width, hidden)), f32),
            pltpu.VMEM((2, length, width), bf16),
            pltpu.VMEM((2, length, hidden), bf16),
            pltpu.VMEM((2, hb, length, c), f32),
            pltpu.VMEM((2, hb, length, c), bf16),
            pltpu.VMEM((2, hb, length, c), bf16),
            pltpu.VMEM((hb, length, c), bf16),
            pltpu.VMEM((hb, length, c), bf16),
            pltpu.VMEM((width // LANES, LANES, 2 * LANES), f32),
            pltpu.VMEM((1, width), f32),
            pltpu.VMEM((8, 2 * hidden), f32),
            dma((max(7, columns // max(c, LANES)),)),
            dma((9, 2, nz)),
            dma((9, 2, nz)),
            dma((9, 2, nz)),
            dma((9, 2, nz)),
            dma((9, nz)),
            dma((9, nz)),
            dma((4,)),
            dma((4,)),
            dma((2, 2, hb)),
            dma((2, 2, hb)),
            dma((2, hb)),
            dma((2, hb)),
            dma((3, hb)),
            dma((3, hb)),
        ],
        compiler_params=pltpu.CompilerParams(
            collective_id=0, has_side_effects=True, vmem_limit_bytes=67_000_000
        ),
        name="layer",
    )(tokens, lru_input, lru_gate, lru_output, ffn_gate, ffn_up, ffn_down, *rest)


def local(mesh_fs, *args):
    (
        tokens,
        mix_gain,
        lru_input,
        lru_gate,
        lru_input_scale,
        lru_gate_scale,
        conv_weight,
        recur_gate,
        input_gate,
        decay_rate,
        extra_decay,
        lru_output,
        lru_output_scale,
        ffn_gain,
        ffn_gate,
        ffn_up,
        ffn_gate_scale,
        ffn_up_scale,
        ffn_down,
        ffn_down_scale,
    ) = args
    ny = 2 if mesh_fs % 2 == 0 else 1
    return layer(
        ny,
        mesh_fs // ny,
        tokens,
        lru_input,
        lru_gate,
        lru_output,
        ffn_gate,
        ffn_up,
        ffn_down,
        extra_decay[None, :],
        mix_gain[None, :],
        ffn_gain[None, :],
        lru_input_scale[None, :],
        lru_gate_scale[None, :],
        lru_output_scale[None, :],
        jnp.stack([ffn_gate_scale, ffn_up_scale]),
        ffn_down_scale[None, :],
        conv_weight,
        recur_gate,
        input_gate,
        decay_rate[None, :],
    )


def solution(mesh):
    in_specs = (
        P(("rep", "fs"), "tp"),
        P(),
        P("fs", "tp"),
        P("fs", "tp"),
        P("tp"),
        P("tp"),
        P(None, "tp"),
        P("tp", None, None),
        P("tp", None, None),
        P("tp"),
        P(("rep", "fs")),
        P("tp", "fs"),
        P(),
        P(),
        P("fs", "tp"),
        P("fs", "tp"),
        P("tp"),
        P("tp"),
        P("tp", "fs"),
        P(),
    )
    out_specs = P(("rep", "fs"), "tp")
    mesh_fs = mesh.shape["fs"]
    return jax.shard_map(
        lambda *args: local(mesh_fs, *args),
        mesh=mesh,
        in_specs=in_specs,
        out_specs=out_specs,
        check_vma=False,
    )
```

```python
import functools

import jax
import jax.numpy as jnp
from jax import lax
from jax.experimental import pallas as pl
from jax.experimental.pallas import tpu as pltpu
from jax.sharding import PartitionSpec as P

EPS = 1e-06
RATE = 8.0
LANES = 128
FIRST = 9.0
RATE_BOTH = 21500.0
EARLY = 4
TOKENS = 39.0
HOP = 22.5
DOT = (1.5, 0.0, 2.2)
MESH = pl.DeviceIdType.MESH


def scoped(name):
    def wrap(f):
        def inner(*args):
            with jax.named_scope(name + "".join(f"_{a}" for a in args if isinstance(a, int))):
                return f(*args)

        return inner

    return wrap


def sigmoid(v):
    return 1.0 / (1.0 + jnp.exp(-v))


def rec_block(values, gate, taps, maps, rate, extra):
    length = values.shape[0]
    ntaps = taps.shape[0]
    row = lax.broadcasted_iota(jnp.int32, values.shape, 0)
    conv = taps[ntaps - 1 : ntaps, :] * values
    for back in range(1, ntaps):
        moved = jnp.where(row >= back, pltpu.roll(values, back, 0), 0.0)
        conv = conv + taps[ntaps - 1 - back : ntaps - back, :] * moved
    mapped = jnp.dot(
        conv, maps, preferred_element_type=jnp.float32, precision=lax.Precision.HIGHEST
    )
    recur = sigmoid(mapped[:, :LANES])
    ingate = sigmoid(mapped[:, LANES:])
    log_rate = rate * recur - extra
    a = jnp.exp(log_rate)
    u = -2.0 * log_rate
    series = u * (1 - u / 2 * (1 - u / 3 * (1 - u / 4 * (1 - u / 5 * (1 - u / 6)))))
    b = jnp.sqrt(jnp.where(u < 0.25, series, 1.0 - jnp.exp(-u))) * (ingate * conv)
    inner = row % 8
    for s in (1, 2, 4):
        keep = inner >= s
        b = jnp.where(keep, a * pltpu.roll(b, s, 0) + b, b)
        a = jnp.where(keep, a * pltpu.roll(a, s, 0), a)
    groups = length // 8
    last_a = a.reshape(groups, 8, LANES)
    last_b = b.reshape(groups, 8, LANES)
    ca = jnp.broadcast_to(last_a[:, 7:8, :], last_a.shape).reshape(length, LANES)
    cb = jnp.broadcast_to(last_b[:, 7:8, :], last_b.shape).reshape(length, LANES)
    s = 8
    while s < length:
        cb_new = ca[s:] * cb[:-s] + cb[s:]
        ca_new = ca[s:] * ca[:-s]
        cb = jnp.concatenate([cb[:s], cb_new], axis=0)
        ca = jnp.concatenate([ca[:s], ca_new], axis=0)
        s *= 2
    state = jnp.concatenate([b[:8], a[8:] * cb[:-8] + b[8:]], axis=0)
    gelu = 0.5 * gate * (1.0 + jnp.tanh(0.7978845608028654 * (gate + 0.044715 * gate * gate * gate)))
    return (state * gelu).astype(jnp.bfloat16)


def layer_kernel(
    ny,
    nz,
    tokens,
    lru_input,
    lru_gate,
    lru_output,
    ffn_gate,
    ffn_up,
    ffn_down,
    extra_ref,
    mgain_ref,
    fgain_ref,
    iscale_ref,
    gscale_ref,
    oscale_ref,
    fscale_ref,
    dscale_ref,
    taps_ref,
    rmap_ref,
    imap_ref,
    decay_ref,
    o_ref,
    tok,
    ex,
    nrm,
    b0,
    b1,
    b2,
    b3,
    give_mix,
    give_out,
    give_gu,
    give_down,
    acc,
    gated,
    hid,
    part,
    thr_s,
    thr_r,
    xr,
    maps,
    rates,
    guscale,
    lsem,
    us,
    ur,
    ds,
    dr,
    ys,
    yr,
    ts,
    tr,
    ps,
    pr,
    xss,
    xrs,
    ms,
    mr,
    free,
):
    f32, bf16 = jnp.float32, jnp.bfloat16
    fs = ny * nz
    length, columns = tokens.shape
    c = lru_input.shape[0]
    hb = columns // c
    width = gated.shape[2]
    hidden = hid.shape[2]
    rep, tp, me = lax.axis_index("rep"), lax.axis_index("tp"), lax.axis_index("fs")
    z, y = me // ny, me % ny
    buf = (b0, b1, b2, b3)
    twin = {"rep": 1 - rep}
    over_tp = {"tp": 1 - tp}
    pair = {"fs": z * ny + (1 - y)}
    give = (give_mix, give_out, give_gu, give_down)
    half = nz // 2
    plan = ((64, 96, 96), (256, 256), (96, 96, 64))
    groups = []
    for b, parts in enumerate(plan):
        row, rows = 0, buf[b].shape[1]
        for i, n in enumerate(parts):
            n = rows - row if i + 1 == len(parts) else max(16, n * rows // sum(parts) // 16 * 16)
            groups.append((b, row, n))
            row += n
    subs = b3.shape[1]
    cs = c // subs
    groups += [(3, i, hidden) for i in range(subs)]

    clock = [0.0]
    eta, slots, at_time = {}, [], FIRST
    for g, (b, _, n) in enumerate(groups):
        size = n * buf[b].shape[-1]
        for k in range(1, nz):
            at_time += size / RATE_BOTH
            eta[g, k] = at_time
            slots.append((g, k))

    def copy(src, dst, s, r, where):
        return pltpu.make_async_remote_copy(
            src_ref=src, dst_ref=dst, send_sem=s, recv_sem=r, device_id=where, device_id_type=MESH
        )

    def cut(g, ref, *at):
        b, row, rows = groups[g]
        return ref.at[(*at, row if b == 3 else pl.ds(row, rows))]

    def piece(g, at, w):
        return cut(g, buf[groups[g][0]], at * ny + (rep if w == 0 else 1 - rep))

    def up(g, k, at):
        p = piece(g, at, 0)
        return copy(p, p, us.at[g, k], ur.at[g, k], {"fs": lax.rem(z + 1, nz) * ny + y})

    def down_z(g, k, at):
        p = piece(g, at, 0)
        return copy(p, p, ds.at[g, k], dr.at[g, k], {"fs": lax.rem(z + nz - 1, nz) * ny + y})

    def from_z(d):
        return lax.rem(z - d + nz, nz)

    def over(g, d, w=0):
        p = piece(g, from_z(d), w)
        return copy(p, p, ys.at[g, d], yr.at[g, d], twin)

    def swap(g):
        b = groups[g][0]
        return copy(cut(g, give[b]), cut(g, buf[b], me), ys.at[g, 0], yr.at[g, 0], pair)

    def can_up(k):
        return (z + 1 < nz) & (z >= k - 1)

    def can_down(k):
        return (z > 0) & (z + k <= nz)

    def own_y(g):
        if g < len(groups):
            swap(g).start()

    def own_z(g):
        if g < len(groups):
            swap(g).wait_recv()

            @pl.when(can_up(1))
            def _():
                up(g, 1, z).start()

            @pl.when(can_down(1))
            def _():
                down_z(g, 1, z).start()

    @scoped("slot")
    def slot(g, k):
        if k == nz - 1 and g <= EARLY:
            own_z(g + 1)
            for n in {2: (5, 6), 3: (7,), 4: (8, 9)}.get(g, ()):
                own_y(n)
            if g == EARLY:
                own_z(g + 2)
        if k == 1 and g > EARLY:
            own_z(g + 2)

        @pl.when(z >= k)
        def _():
            up(g, k, z - k).wait_recv()
            if k + 1 < nz:

                @pl.when(can_up(k + 1))
                def _():
                    up(g, k + 1, z - k).start()

            over(g, k).start()

        @pl.when(z + k < nz)
        def _():
            down_z(g, k, z + k).wait_recv()
            if k + 1 < nz:

                @pl.when(can_down(k + 1))
                def _():
                    down_z(g, k + 1, z + k).start()

            over(g, nz - k).start()

    def next_slot():
        key = slots.pop(0)
        clock[0] = max(clock[0], eta[key])
        slot(*key)

    def pump(until):
        while slots and eta[slots[0]] <= until:
            next_slot()

    def need(b, k):
        g = max(i for i, group in enumerate(groups) if group[0] == b)
        while slots and slots[0] <= (g, k):
            next_slot()

    def run(cost, f, *args):
        pump(clock[0] + cost / 2)
        f(*args)
        clock[0] += cost

    def wait_until(when, f, *args):
        pump(when)
        f(*args)
        clock[0] = max(clock[0], when)

    def nth(i):
        near = jnp.minimum(z, nz - 1 - z)
        step = i // 2 + 1
        both = z - step if i % 2 == 0 else z + step
        far = i - near + 1
        rest = jnp.where(z > nz - 1 - z, z - far, z + far)
        return jnp.where(i < 2 * near, both, rest)

    def stage(src, dst, i):
        return pltpu.make_async_copy(src, dst, lsem.at[i])

    mine_cols = pl.ds(pl.multiple_of(y * width, LANES), width)
    give_cols = pl.ds(pl.multiple_of((1 - y) * width, LANES), width)
    cuts = range(0, hidden, length)
    loads = [
        stage(lru_input, acc.at[0, c : 2 * c, : 2 * width], 0),
        stage(lru_gate, acc.at[1, c : 2 * c, : 2 * width], 1),
        stage(tokens, tok.at[0, tp], 2),
        stage(ffn_gate, acc.at[0, :c], 3),
        stage(ffn_up, acc.at[1, :c], 4),
    ]
    for h in range(2):
        for i in range(subs):
            cols = pl.ds(i * cs, cs)
            src = lru_output.at[pl.ds(h * width, width), cols]
            loads.append(stage(src, part.at[0, h * subs + i, :width], len(loads)))
    for h in range(2):
        for i in range(subs):
            for r, row in enumerate(cuts):
                n = min(length, hidden - row)
                src = ffn_down.at[pl.ds(h * hidden + row, n), pl.ds(i * cs, cs)]
                to = part.at[1, (h * subs + i) * len(cuts) + r, :n]
                loads.append(stage(src, to, len(loads)))
    for load in loads:
        load.start()

    barrier = pltpu.get_barrier_semaphore()

    def greet(where):
        pl.semaphore_signal(barrier, inc=1, device_id=where, device_id_type=MESH)

    greet(pair)
    greet(twin)
    greet(over_tp)
    pl.when(z + 1 < nz)(lambda: greet({"fs": lax.rem(z + 1, nz) * ny + y}))
    pl.when(z > 0)(lambda: greet({"fs": lax.rem(z + nz - 1, nz) * ny + y}))

    loads[0].wait()
    loads[1].wait()
    for i in range(2):
        cols = slice(i * width, (i + 1) * width)
        give_mix[:, cols] = acc[i, c : 2 * c, give_cols].astype(bf16)
        b0[me, :, cols] = acc[i, c : 2 * c, mine_cols].astype(bf16)
    ex[0] = jnp.broadcast_to(extra_ref[...], ex.shape[1:])
    loads[2].wait()

    along_z = jnp.where(z > 0, 1, 0) + jnp.where(z + 1 < nz, 1, 0)
    pl.semaphore_wait(barrier, 3 + along_z)

    def tok_copy(s, i, where, to):
        return copy(tok.at[s, tp], tok.at[to, tp], ts.at[i], tr.at[i], where)

    tok_tp = tok_copy(0, 0, over_tp, 0)
    tok_x = tok_copy(0, 1, pair, 1)
    tok_xtp = tok_copy(1, 2, over_tp, 1)
    extra_x = copy(ex.at[0], ex.at[1], ts.at[3], tr.at[3], pair)
    own_y(0)
    tok_tp.start()
    extra_x.start()
    for load in loads[5 : 5 + 2 * subs]:
        load.wait()
    for i in range(subs):
        cols = slice(i * cs, (i + 1) * cs)
        b1[me, :, cols] = part[0, y * subs + i, :width].astype(bf16)
        give_out[:, cols] = part[0, (1 - y) * subs + i, :width].astype(bf16)
    own_y(1)
    own_y(2)
    own_z(0)

    @scoped("wait")
    def arrived(c):
        c.wait_recv()

    main = hidden // LANES * LANES
    rest = hidden - main

    @scoped("pack")
    def pack():
        loads[3].wait()
        loads[4].wait()
        step = 32

        def half_of(v, which):
            return jnp.where(which == 0, v, pltpu.roll(v, hidden, 1))

        def joined(g, u, which):
            g, u = half_of(g, which), half_of(u, which)
            out = [g[:, :main], u[:, :main]]
            if rest:
                g, u = g[:, main : main + LANES], u[:, main : main + LANES]
                lane = lax.broadcasted_iota(jnp.int32, g.shape, 1)
                out.append(jnp.where(lane < rest, g, pltpu.roll(u, rest, 1)))
            return out

        def body(i, _):
            r = pl.ds(pl.multiple_of(i * step, step), step)
            for which, to in ((y, b2.at[me]), (1 - y, give_gu)):
                out = joined(acc[0, r, :], acc[1, r, :], which)
                to[r, :main] = out[0].astype(bf16)
                to[r, main : 2 * main] = out[1].astype(bf16)
                if rest:
                    to[r, 2 * main :] = out[2].astype(bf16)
            return 0

        lax.fori_loop(0, c // step, body, 0)
        wide = (8, 2 * hidden)
        out = joined(
            jnp.broadcast_to(fscale_ref[0:1, :], wide),
            jnp.broadcast_to(fscale_ref[1:2, :], wide),
            y,
        )
        guscale[:, :main] = out[0]
        guscale[:, main : 2 * main] = out[1]
        if rest:
            guscale[:, 2 * main :] = out[2]
        for load in loads[5 + 2 * subs :]:
            load.wait()
        for i in range(subs):
            for which, to in ((y, b3.at[me, i]), (1 - y, give_down.at[i])):
                for r, row in enumerate(cuts):
                    n = min(length, hidden - row)
                    at = (which * subs + i) * len(cuts) + r
                    to[row : row + n] = part[1, at, :n].astype(bf16)

    @scoped("tables")
    def tables():
        v = -decay_ref[:, mine_cols]
        e = jnp.exp(-jnp.abs(v))
        q = e / (2.0 + e)
        p = q * q
        poly = jnp.full_like(p, 1.0 / 17)
        for odd in range(15, 0, -2):
            poly = poly * p + 1.0 / odd
        rates[...] = -RATE * (jnp.maximum(v, 0.0) + 2.0 * q * poly)
        bdim = rmap_ref.shape[1]
        per = LANES // bdim
        zero = jnp.zeros((bdim, bdim), f32)
        for i in range(width // LANES):
            for p_ in range(per):
                for k, ref in enumerate((rmap_ref, imap_ref)):
                    block = ref[y * (width // bdim) + i * per + p_]
                    maps[i, p_ * bdim : (p_ + 1) * bdim, k * LANES : (k + 1) * LANES] = (
                        jnp.concatenate(
                            [block if q_ == p_ else zero for q_ in range(per)], axis=1
                        )
                    )

    @scoped("norm")
    def norm(read, s, gain):
        step = 128

        def body(i, _):
            r = pl.ds(pl.multiple_of(i * step, step), step)
            total = jnp.zeros((step, 1), f32)
            for b in range(fs):
                v = read(b, r).astype(f32)
                total = total + jnp.sum(v * v, axis=-1, keepdims=True)
            scale = lax.rsqrt(total / (fs * c) + EPS)
            for b in range(fs):
                v = read(b, r).astype(f32)
                nrm[s, b, r, :] = (v * scale * gain[:, b * c : (b + 1) * c]).astype(bf16)
            return 0

        lax.fori_loop(0, length // step, body, 0)

    def tok_block(s):
        return lambda b, r: tok[s, b // hb, r, b % hb * c : (b % hb + 1) * c]

    @scoped("dot")
    def dot(b, s, at, first):
        n = buf[b].shape[2]
        tile = 256
        src = pl.ds(at * ny, ny)
        rows = jnp.concatenate([nrm[s, at * ny + i] for i in range(ny)], axis=1)

        def one(cols):
            v = jnp.dot(
                rows, buf[b][src, :, cols].reshape(ny * c, -1), preferred_element_type=f32
            )
            if first:
                acc[s, :, cols] = v
            else:
                acc[s, :, cols] += v

        def body(i, _):
            one(pl.ds(pl.multiple_of(i * tile, tile), tile))
            return 0

        lax.fori_loop(0, n // tile, body, 0)
        if n % tile:
            one(pl.ds(n // tile * tile, n % tile))

    def from_twin(b, d, sub=0):
        for g, group in enumerate(groups):
            if group[0] == b and (b < 3 or group[1] == sub):
                arrived(over(g, d, 1))

    def ready(b, i):
        need(b, i + 1)
        if i >= 0:
            from_twin(b, lax.rem(z - nth(i) + nz, nz))

    def dots(b, s, i):
        run(DOT[b], dot, b, s, z if i < 0 else nth(i), i < 0)

    @scoped("recur")
    def recurrence(s, lo, hi):
        extra = jnp.transpose(ex[s])[:, :1]

        def body(i, _):
            lanes = pl.ds(pl.multiple_of(i * LANES, LANES), LANES)
            glanes = pl.ds(pl.multiple_of(width + i * LANES, LANES), LANES)
            wide = pl.ds(pl.multiple_of(y * width + i * LANES, LANES), LANES)
            values = (acc[s, :, lanes] * iscale_ref[:, wide]).astype(bf16).astype(f32)
            gate = (acc[s, :, glanes] * gscale_ref[:, wide]).astype(bf16).astype(f32)
            gated[s, :, lanes] = rec_block(
                values, gate, taps_ref[:, wide], maps[i], rates[:, lanes], extra
            )
            return 0

        lax.fori_loop(lo, hi, body, 0)

    def part_of(j, i):
        return pl.ds(j * subs, subs) if i is None else pl.ds(j * subs + i, 1)

    def tp_copy(l, s, j, i=None):
        at, sem = part_of(j, i), j * subs + (i or 0)
        return copy(thr_s.at[s, at], thr_r.at[s, at], ps.at[l, s, sem], pr.at[l, s, sem], over_tp)

    def x_copy(l, s, j, i=None):
        at, sem = part_of(j, i), j * subs + (i or 0)
        return copy(
            thr_s.at[s, at], xr.at[1 - s, at], xss.at[l, s, sem], xrs.at[l, 1 - s, sem], pair
        )

    def x_arrived(l, s, j, i=None):
        x_copy(l, 1 - s, j, i).wait_recv()

    @scoped("project")
    def project(l, s, j, i=None):
        theirs, mine = (1 - tp) * hb + j, tp * hb + j

        def product(at):
            acts, w = (gated, b1.at[at]) if l == 0 else (hid, b3.at[at, i])
            return jnp.dot(acts[s], w[...], preferred_element_type=f32)

        def put(to, v):
            for k in range(subs) if i is None else (i,):
                cols = slice(k * cs, (k + 1) * cs) if i is None else slice(0, cs)
                to[s, j * subs + k] = v[:, cols].astype(to.dtype)

        put(thr_s, product(theirs))
        tp_copy(l, s, j, i).start()
        put(part, product(mine))

    @scoped("send")
    def send(l, s, j, i=None):
        tp_copy(l, s, j, i).wait()
        at = part_of(j, i)
        total = part[s, at] + thr_r[s, at].astype(f32)
        thr_s[s, at] = total.astype(bf16)
        x_copy(l, s, j, i).start()
        if l == 0:
            part[s, at] = total

    def residual(scale, s, j, k):
        at = j * subs + k
        total = part[s, at] + xr[s, at].astype(f32)
        if scale is dscale_ref:
            total = total + thr_r[s, at].astype(f32)
        lo = j * c + k * cs
        cols = slice(lo, lo + cs)
        factor = jnp.where(
            tp == 0, scale[:, cols], scale[:, columns + lo : columns + lo + cs]
        )
        tok[s, tp, :, cols] = (tok[s, tp, :, cols].astype(f32) + total * factor).astype(bf16)

    chunk = max(c, LANES)
    chunks = columns // chunk

    def m_tp(s, q):
        at = tok.at[s, tp, :, pl.ds(q * chunk, chunk)]
        return copy(at, at, ms.at[s, q], mr.at[s, q], over_tp)

    @scoped("mixed")
    def mixed(s, q):
        for j in range(q * chunk // c, (q + 1) * chunk // c):
            x_arrived(0, s, j)
            for k in range(subs):
                residual(oscale_ref, s, j, k)
        m_tp(s, q).start()

    @scoped("hide")
    def hide(s):
        def silu_up(g, u):
            return (g / (1.0 + jnp.exp(-g)) * u).astype(bf16)

        def body(i, _):
            step = 128
            r = pl.ds(pl.multiple_of(i * step, step), step)
            for k in range(0, main, LANES):
                m = main + k
                g = acc[s, r, k : k + LANES] * guscale[0:1, k : k + LANES]
                u = acc[s, r, m : m + LANES] * guscale[0:1, m : m + LANES]
                hid[s, r, k : k + LANES] = silu_up(g, u)
            if rest:
                both = acc[s, r, 2 * main :] * guscale[0:1, 2 * main :]
                hid[s, r, main:] = silu_up(both, pltpu.roll(both, rest, 1))[:, :rest]
            return 0

        lax.fori_loop(0, length // 128, body, 0)

    def store(q):
        cols = pl.ds(q * chunk, chunk)
        return pltpu.make_async_copy(tok.at[0, tp, :, cols], o_ref.at[:, cols], lsem.at[q])

    @scoped("finish")
    def finish(q):
        m_tp(0, q).wait_send()
        for j in range(q * chunk // c, (q + 1) * chunk // c):
            for k in range(subs):
                tp_copy(1, 0, j, k).wait_recv()
                x_arrived(1, 0, j, k)
                residual(dscale_ref, 0, j, k)
        store(q).start()

    ranks = range(-1, nz - 1)
    blocks = width // LANES
    spans = [(lo, min(lo + 2, blocks)) for lo in range(0, blocks, 2)]
    wait_until(6.0, arrived, tok_tp)
    run(1.3, norm, tok_block(0), 0, mgain_ref)
    next_slot()
    tok_x.start()
    run(1.4, pack)
    run(1.0, tables)
    wait_until(TOKENS, arrived, tok_x)
    tok_xtp.start()
    own_y(3)
    own_y(4)
    wait_until(TOKENS + 3.0, arrived, tok_xtp)
    run(1.3, norm, tok_block(1), 1, mgain_ref)
    for sent in (tok_tp, tok_x, tok_xtp, extra_x):
        sent.wait_send()
    ready(0, -1)
    for s in (0, 1):
        dots(0, s, -1)
    for i in ranks[1:]:
        ready(0, i)
        for s in (0, 1):
            dots(0, s, i)
    arrived(extra_x)
    for s in (1, 0):
        for span in spans:
            run(3.3, recurrence, s, *span)
    for i in ranks:
        ready(1, i)
    for s in (1, 0):
        for j in range(hb):
            run(0.9, project, 0, s, j)
            if j:
                run(0.4, send, 0, s, j - 1)
        run(0.4, send, 0, s, hb - 1)
    start = clock[0] - 8
    for s in (0, 1):
        for q in range(chunks):
            wait_until(start + HOP * (s + (q + 1) / chunks), mixed, s, q)
        if s == 0:
            pl.semaphore_signal(free, inc=1, device_id=pair, device_id_type=MESH)
        else:
            ready(2, -1)
            dots(2, 0, -1)
        for q in range(chunks):
            arrived(m_tp(s, q))
        run(1.3, norm, tok_block(s), s, fgain_ref)
    dots(2, 1, -1)
    for i in ranks[1:]:
        ready(2, i)
        for s in (1, 0):
            dots(2, s, i)
    run(0.8, hide, 1)
    run(0.8, hide, 0)
    for j in range(hb):
        for s in range(2):
            x_copy(0, s, j).wait_send()
    pl.semaphore_wait(free, 1)

    for i in range(subs):
        g = len(groups) - subs + i
        for w in (0, 1):
            for k in range(half):
                d = half if k == 0 and w == 0 else nz - 1
                while slots and slots[0] <= (g, d):
                    next_slot()
                if w:
                    if k:
                        from_twin(3, k, i)
                    from_twin(3, k + half, i)
                j = lax.rem(z - k + nz, half) * ny + (1 - rep if w else rep)
                run(0.4, project, 1, 1, j, i)
                run(0.4, project, 1, 0, j, i)
                run(0.3, send, 1, 1, j, i)
    for q in range(chunks):
        finish(q)

    @scoped("sent")
    def sent_all():
        for g in range(len(groups)):
            for k in range(1, nz):

                @pl.when(can_up(k))
                def _():
                    up(g, k, z - k + 1).wait_send()

                @pl.when(can_down(k))
                def _():
                    down_z(g, k, z + k - 1).wait_send()

                over(g, k).wait_send()
            swap(g).wait_send()
        for j in range(hb):
            for i in range(subs):
                x_copy(1, 1, j, i).wait_send()
                tp_copy(1, 0, j, i).wait_send()
        for q in range(chunks):
            m_tp(1, q).wait_send()

    @scoped("stored")
    def stored():
        for q in range(chunks):
            store(q).wait()

    sent_all()
    stored()


def layer(ny, nz, tokens, lru_input, lru_gate, lru_output, ffn_gate, ffn_up, ffn_down, *rest):
    fs = ny * nz
    length, columns = tokens.shape
    c = lru_input.shape[0]
    hb = columns // c
    width, hidden = lru_output.shape[0] // 2, ffn_down.shape[0] // 2
    subs = 2 if c % (2 * LANES) == 0 else 1
    cut = (hb * subs, length, c // subs)
    bf16, f32 = jnp.bfloat16, jnp.float32
    dma = pltpu.SemaphoreType.DMA
    vmem = pl.BlockSpec(memory_space=pltpu.VMEM)
    hbm = pl.BlockSpec(memory_space=pl.ANY)
    return pl.pallas_call(
        functools.partial(layer_kernel, ny, nz),
        out_shape=jax.ShapeDtypeStruct((length, columns), bf16),
        in_specs=[hbm] * 7 + [vmem] * len(rest),
        out_specs=hbm,
        scratch_shapes=[
            pltpu.VMEM((2, 2, length, columns), bf16),
            pltpu.VMEM((2, 8, length), f32),
            pltpu.VMEM((2, fs, length, c), bf16),
            pltpu.VMEM((fs, c, 2 * width), bf16),
            pltpu.VMEM((fs, width, c), bf16),
            pltpu.VMEM((fs, c, 2 * hidden), bf16),
            pltpu.VMEM((fs, subs, hidden, c // subs), bf16),
            pltpu.VMEM((c, 2 * width), bf16),
            pltpu.VMEM((width, c), bf16),
            pltpu.VMEM((c, 2 * hidden), bf16),
            pltpu.VMEM((subs, hidden, c // subs), bf16),
            pltpu.VMEM((2, length, 2 * max(width, hidden)), f32),
            pltpu.VMEM((2, length, width), bf16),
            pltpu.VMEM((2, length, hidden), bf16),
            pltpu.VMEM((2, *cut), f32),
            pltpu.VMEM((2, *cut), bf16),
            pltpu.VMEM((2, *cut), bf16),
            pltpu.VMEM((2, *cut), bf16),
            pltpu.VMEM((width // LANES, LANES, 2 * LANES), f32),
            pltpu.VMEM((1, width), f32),
            pltpu.VMEM((8, 2 * hidden), f32),
            dma((max(32, columns // LANES),)),
            dma((10, nz)),
            dma((10, nz)),
            dma((10, nz)),
            dma((10, nz)),
            dma((10, nz)),
            dma((10, nz)),
            dma((4,)),
            dma((4,)),
            dma((2, 2, cut[0])),
            dma((2, 2, cut[0])),
            dma((2, 2, cut[0])),
            dma((2, 2, cut[0])),
            dma((2, hb)),
            dma((2, hb)),
            pltpu.SemaphoreType.REGULAR,
        ],
        compiler_params=pltpu.CompilerParams(
            collective_id=0, has_side_effects=True, vmem_limit_bytes=67_000_000
        ),
        name="layer",
    )(tokens, lru_input, lru_gate, lru_output, ffn_gate, ffn_up, ffn_down, *rest)


def local(mesh_fs, *args):
    (
        tokens,
        mix_gain,
        lru_input,
        lru_gate,
        lru_input_scale,
        lru_gate_scale,
        conv_weight,
        recur_gate,
        input_gate,
        decay_rate,
        extra_decay,
        lru_output,
        lru_output_scale,
        ffn_gain,
        ffn_gate,
        ffn_up,
        ffn_gate_scale,
        ffn_up_scale,
        ffn_down,
        ffn_down_scale,
    ) = args
    ny = 2 if mesh_fs % 2 == 0 else 1
    return layer(
        ny,
        mesh_fs // ny,
        tokens,
        lru_input,
        lru_gate,
        lru_output,
        ffn_gate,
        ffn_up,
        ffn_down,
        extra_decay[None, :],
        mix_gain[None, :],
        ffn_gain[None, :],
        lru_input_scale[None, :],
        lru_gate_scale[None, :],
        lru_output_scale[None, :],
        jnp.stack([ffn_gate_scale, ffn_up_scale]),
        ffn_down_scale[None, :],
        conv_weight,
        recur_gate,
        input_gate,
        decay_rate[None, :],
    )


def solution(mesh):
    in_specs = (
        P(("rep", "fs"), "tp"),
        P(),
        P("fs", "tp"),
        P("fs", "tp"),
        P("tp"),
        P("tp"),
        P(None, "tp"),
        P("tp", None, None),
        P("tp", None, None),
        P("tp"),
        P(("rep", "fs")),
        P("tp", "fs"),
        P(),
        P(),
        P("fs", "tp"),
        P("fs", "tp"),
        P("tp"),
        P("tp"),
        P("tp", "fs"),
        P(),
    )
    out_specs = P(("rep", "fs"), "tp")
    mesh_fs = mesh.shape["fs"]
    return jax.shard_map(
        lambda *args: local(mesh_fs, *args),
        mesh=mesh,
        in_specs=in_specs,
        out_specs=out_specs,
        check_vma=False,
    )
```

```python
import functools

import jax
import jax.numpy as jnp
from jax import lax
from jax.experimental import pallas as pl
from jax.experimental.pallas import tpu as pltpu
from jax.sharding import PartitionSpec as P

EPS = 1e-06
RATE = 8.0
LANES = 128
FIRST = 9.0
RATE_BOTH = 21500.0
EARLY = 4
TOKENS = 39.0
LAG = 0.0
HOP = 22.5
DOT = (1.5, 0.0, 2.2)
MESH = pl.DeviceIdType.MESH


def scoped(name):
    def wrap(f):
        def inner(*args):
            with jax.named_scope(name + "".join(f"_{a}" for a in args if isinstance(a, int))):
                return f(*args)

        return inner

    return wrap


def sigmoid(v):
    return 1.0 / (1.0 + jnp.exp(-v))


def rec_block(values, gate, taps, maps, rate, extra):
    length = values.shape[0]
    ntaps = taps.shape[0]
    row = lax.broadcasted_iota(jnp.int32, values.shape, 0)
    conv = taps[ntaps - 1 : ntaps, :] * values
    for back in range(1, ntaps):
        moved = jnp.where(row >= back, pltpu.roll(values, back, 0), 0.0)
        conv = conv + taps[ntaps - 1 - back : ntaps - back, :] * moved
    mapped = jnp.dot(
        conv, maps, preferred_element_type=jnp.float32, precision=lax.Precision.HIGHEST
    )
    recur = sigmoid(mapped[:, :LANES])
    ingate = sigmoid(mapped[:, LANES:])
    log_rate = rate * recur - extra
    a = jnp.exp(log_rate)
    u = -2.0 * log_rate
    series = u * (1 - u / 2 * (1 - u / 3 * (1 - u / 4 * (1 - u / 5 * (1 - u / 6)))))
    b = jnp.sqrt(jnp.where(u < 0.25, series, 1.0 - jnp.exp(-u))) * (ingate * conv)
    inner = row % 8
    for s in (1, 2, 4):
        keep = inner >= s
        b = jnp.where(keep, a * pltpu.roll(b, s, 0) + b, b)
        a = jnp.where(keep, a * pltpu.roll(a, s, 0), a)
    groups = length // 8
    last_a = a.reshape(groups, 8, LANES)
    last_b = b.reshape(groups, 8, LANES)
    ca = jnp.broadcast_to(last_a[:, 7:8, :], last_a.shape).reshape(length, LANES)
    cb = jnp.broadcast_to(last_b[:, 7:8, :], last_b.shape).reshape(length, LANES)
    s = 8
    while s < length:
        cb_new = ca[s:] * cb[:-s] + cb[s:]
        ca_new = ca[s:] * ca[:-s]
        cb = jnp.concatenate([cb[:s], cb_new], axis=0)
        ca = jnp.concatenate([ca[:s], ca_new], axis=0)
        s *= 2
    state = jnp.concatenate([b[:8], a[8:] * cb[:-8] + b[8:]], axis=0)
    gelu = 0.5 * gate * (1.0 + jnp.tanh(0.7978845608028654 * (gate + 0.044715 * gate * gate * gate)))
    return (state * gelu).astype(jnp.bfloat16)


def layer_kernel(
    ny,
    nz,
    tokens,
    lru_input,
    lru_gate,
    lru_output,
    ffn_gate,
    ffn_up,
    ffn_down,
    extra_ref,
    mgain_ref,
    fgain_ref,
    iscale_ref,
    gscale_ref,
    oscale_ref,
    fscale_ref,
    dscale_ref,
    taps_ref,
    rmap_ref,
    imap_ref,
    decay_ref,
    o_ref,
    tok,
    ex,
    nrm,
    b0,
    b1,
    b2,
    b3,
    give_mix,
    give_out,
    give_gu,
    give_down,
    acc,
    gated,
    hid,
    part,
    thr_s,
    thr_r,
    xr,
    maps,
    rates,
    guscale,
    lsem,
    us,
    ur,
    ds,
    dr,
    ys,
    yr,
    ts,
    tr,
    ps,
    pr,
    xss,
    xrs,
    ms,
    mr,
    free,
):
    f32, bf16 = jnp.float32, jnp.bfloat16
    fs = ny * nz
    length, columns = tokens.shape
    c = lru_input.shape[0]
    hb = columns // c
    width = gated.shape[2]
    hidden = hid.shape[2]
    rep, tp, me = lax.axis_index("rep"), lax.axis_index("tp"), lax.axis_index("fs")
    z, y = me // ny, me % ny
    buf = (b0, b1, b2, b3)
    twin = {"rep": 1 - rep}
    over_tp = {"tp": 1 - tp}
    pair = {"fs": z * ny + (1 - y)}
    give = (give_mix, give_out, give_gu, give_down)
    half = nz // 2
    plan = ((64, 96, 96), (256, 256), (96, 96, 64), (352, 352))
    groups = []
    for b, parts in enumerate(plan):
        row, rows = 0, buf[b].shape[-2]
        for i, n in enumerate(parts):
            n = rows - row if i + 1 == len(parts) else max(16, n * rows // sum(parts) // 16 * 16)
            groups.append((b, row, n))
            row += n
    subs = part.shape[1] // hb
    cs = c // subs

    clock = [0.0]
    eta, slots, at_time = {}, [], FIRST
    for g, (b, _, n) in enumerate(groups):
        size = n * buf[b].shape[-1]
        at_time += LAG if g == EARLY + 1 else 0.0
        for k in range(1, nz):
            at_time += size / RATE_BOTH
            eta[g, k] = at_time
            slots.append((g, k))

    def copy(src, dst, s, r, where):
        return pltpu.make_async_remote_copy(
            src_ref=src, dst_ref=dst, send_sem=s, recv_sem=r, device_id=where, device_id_type=MESH
        )

    def cut(g, ref, *at):
        b, row, rows = groups[g]
        return ref.at[(*at, pl.ds(row, rows))]

    def piece(g, at, w):
        return cut(g, buf[groups[g][0]], at * ny + (rep if w == 0 else 1 - rep))

    def up(g, k, at):
        p = piece(g, at, 0)
        return copy(p, p, us.at[g, k], ur.at[g, k], {"fs": lax.rem(z + 1, nz) * ny + y})

    def down_z(g, k, at):
        p = piece(g, at, 0)
        return copy(p, p, ds.at[g, k], dr.at[g, k], {"fs": lax.rem(z + nz - 1, nz) * ny + y})

    def from_z(d):
        return lax.rem(z - d + nz, nz)

    def over(g, d, w=0):
        p = piece(g, from_z(d), w)
        return copy(p, p, ys.at[g, d], yr.at[g, d], twin)

    def swap(g):
        b = groups[g][0]
        return copy(cut(g, give[b]), cut(g, buf[b], me), ys.at[g, 0], yr.at[g, 0], pair)

    def can_up(k):
        return (z + 1 < nz) & (z >= k - 1)

    def can_down(k):
        return (z > 0) & (z + k <= nz)

    def own_y(g):
        if g < len(groups):
            swap(g).start()

    def own_z(g):
        if g < len(groups):
            swap(g).wait_recv()

            @pl.when(can_up(1))
            def _():
                up(g, 1, z).start()

            @pl.when(can_down(1))
            def _():
                down_z(g, 1, z).start()

    @scoped("slot")
    def slot(g, k):
        if k == nz - 1:
            for n in {2: (5, 6), 3: (7,), 4: (8, 9)}.get(g, ()):
                own_y(n)

        @pl.when(z >= k)
        def _():
            up(g, k, z - k).wait_recv()
            if k + 1 < nz:

                @pl.when(can_up(k + 1))
                def _():
                    up(g, k + 1, z - k).start()

            over(g, k).start()

        @pl.when(z + k < nz)
        def _():
            down_z(g, k, z + k).wait_recv()
            if k + 1 < nz:

                @pl.when(can_down(k + 1))
                def _():
                    down_z(g, k + 1, z + k).start()

            over(g, nz - k).start()

        if k == (max(1, nz - 2) if g <= EARLY else 1):
            own_z(g + 1)

    def next_slot():
        key = slots.pop(0)
        clock[0] = max(clock[0], eta[key])
        slot(*key)

    def pump(until):
        while slots and eta[slots[0]] <= until:
            next_slot()

    def need(b, k):
        g = max(i for i, group in enumerate(groups) if group[0] == b)
        while slots and slots[0] <= (g, k):
            next_slot()

    def run(cost, f, *args):
        pump(clock[0] + cost / 2)
        f(*args)
        clock[0] += cost

    def wait_until(when, f, *args):
        pump(when)
        f(*args)
        clock[0] = max(clock[0], when)

    def nth(i):
        near = jnp.minimum(z, nz - 1 - z)
        step = i // 2 + 1
        both = z - step if i % 2 == 0 else z + step
        far = i - near + 1
        rest = jnp.where(z > nz - 1 - z, z - far, z + far)
        return jnp.where(i < 2 * near, both, rest)

    def stage(src, dst, i):
        return pltpu.make_async_copy(src, dst, lsem.at[i])

    mine_cols = pl.ds(pl.multiple_of(y * width, LANES), width)
    give_cols = pl.ds(pl.multiple_of((1 - y) * width, LANES), width)
    cuts = range(0, hidden, length)
    loads = [
        stage(lru_input, acc.at[0, c : 2 * c, : 2 * width], 0),
        stage(lru_gate, acc.at[1, c : 2 * c, : 2 * width], 1),
        stage(tokens, tok.at[0, tp], 2),
        stage(ffn_gate, acc.at[0, :c], 3),
        stage(ffn_up, acc.at[1, :c], 4),
    ]
    for h in range(2):
        for i in range(subs):
            cols = pl.ds(i * cs, cs)
            src = lru_output.at[pl.ds(h * width, width), cols]
            loads.append(stage(src, part.at[0, h * subs + i, :width], len(loads)))
    for h in range(2):
        for i in range(subs):
            for r, row in enumerate(cuts):
                n = min(length, hidden - row)
                src = ffn_down.at[pl.ds(h * hidden + row, n), pl.ds(i * cs, cs)]
                to = part.at[1, (h * subs + i) * len(cuts) + r, :n]
                loads.append(stage(src, to, len(loads)))
    barrier = pltpu.get_barrier_semaphore()

    def greet(where):
        pl.semaphore_signal(barrier, inc=1, device_id=where, device_id_type=MESH)

    greet(pair)
    greet(twin)
    greet(over_tp)
    pl.when(z + 1 < nz)(lambda: greet({"fs": lax.rem(z + 1, nz) * ny + y}))
    pl.when(z > 0)(lambda: greet({"fs": lax.rem(z + nz - 1, nz) * ny + y}))

    for load in loads[:3]:
        load.start()
    loads[0].wait()
    loads[1].wait()
    for i in range(2):
        cols = slice(i * width, (i + 1) * width)
        give_mix[:, cols] = acc[i, c : 2 * c, give_cols].astype(bf16)
        b0[me, :, cols] = acc[i, c : 2 * c, mine_cols].astype(bf16)
    ex[0] = jnp.broadcast_to(extra_ref[...], ex.shape[1:])
    loads[2].wait()

    along_z = jnp.where(z > 0, 1, 0) + jnp.where(z + 1 < nz, 1, 0)
    pl.semaphore_wait(barrier, 3 + along_z)

    def tok_copy(s, i, where, to):
        return copy(tok.at[s, tp], tok.at[to, tp], ts.at[i], tr.at[i], where)

    tok_tp = tok_copy(0, 0, over_tp, 0)
    tok_x = tok_copy(0, 1, pair, 1)
    tok_xtp = tok_copy(1, 2, over_tp, 1)
    extra_x = copy(ex.at[0], ex.at[1], ts.at[3], tr.at[3], pair)
    own_y(0)
    tok_tp.start()
    for load in loads[5:] + loads[3:5]:
        load.start()
    extra_x.start()
    for load in loads[5 : 5 + 2 * subs]:
        load.wait()
    for i in range(subs):
        cols = slice(i * cs, (i + 1) * cs)
        b1[me, :, cols] = part[0, y * subs + i, :width].astype(bf16)
        give_out[:, cols] = part[0, (1 - y) * subs + i, :width].astype(bf16)
    own_y(1)
    own_y(2)
    own_z(0)

    @scoped("wait")
    def arrived(c):
        c.wait_recv()

    main = hidden // LANES * LANES
    rest = hidden - main

    @scoped("pack")
    def pack():
        loads[3].wait()
        loads[4].wait()
        step = 32

        def half_of(v, which):
            return jnp.where(which == 0, v, pltpu.roll(v, hidden, 1))

        def joined(g, u, which):
            g, u = half_of(g, which), half_of(u, which)
            out = [g[:, :main], u[:, :main]]
            if rest:
                g, u = g[:, main : main + LANES], u[:, main : main + LANES]
                lane = lax.broadcasted_iota(jnp.int32, g.shape, 1)
                out.append(jnp.where(lane < rest, g, pltpu.roll(u, rest, 1)))
            return out

        def body(i, _):
            r = pl.ds(pl.multiple_of(i * step, step), step)
            for which, to in ((y, b2.at[me]), (1 - y, give_gu)):
                out = joined(acc[0, r, :], acc[1, r, :], which)
                to[r, :main] = out[0].astype(bf16)
                to[r, main : 2 * main] = out[1].astype(bf16)
                if rest:
                    to[r, 2 * main :] = out[2].astype(bf16)
            return 0

        lax.fori_loop(0, c // step, body, 0)
        wide = (8, 2 * hidden)
        out = joined(
            jnp.broadcast_to(fscale_ref[0:1, :], wide),
            jnp.broadcast_to(fscale_ref[1:2, :], wide),
            y,
        )
        guscale[:, :main] = out[0]
        guscale[:, main : 2 * main] = out[1]
        if rest:
            guscale[:, 2 * main :] = out[2]
        for load in loads[5 + 2 * subs :]:
            load.wait()
        for i in range(subs):
            for which, to in ((y, b3.at[me]), (1 - y, give_down)):
                for r, row in enumerate(cuts):
                    n = min(length, hidden - row)
                    at = (which * subs + i) * len(cuts) + r
                    to[row : row + n, i * cs : (i + 1) * cs] = part[1, at, :n].astype(bf16)

    @scoped("tables")
    def tables():
        v = -decay_ref[:, mine_cols]
        e = jnp.exp(-jnp.abs(v))
        q = e / (2.0 + e)
        p = q * q
        poly = jnp.full_like(p, 1.0 / 17)
        for odd in range(15, 0, -2):
            poly = poly * p + 1.0 / odd
        rates[...] = -RATE * (jnp.maximum(v, 0.0) + 2.0 * q * poly)
        bdim = rmap_ref.shape[1]
        per = LANES // bdim
        zero = jnp.zeros((bdim, bdim), f32)
        for i in range(width // LANES):
            for p_ in range(per):
                for k, ref in enumerate((rmap_ref, imap_ref)):
                    block = ref[y * (width // bdim) + i * per + p_]
                    maps[i, p_ * bdim : (p_ + 1) * bdim, k * LANES : (k + 1) * LANES] = (
                        jnp.concatenate(
                            [block if q_ == p_ else zero for q_ in range(per)], axis=1
                        )
                    )

    @scoped("norm")
    def norm(read, s, gain):
        step = 128

        def body(i, _):
            r = pl.ds(pl.multiple_of(i * step, step), step)
            total = jnp.zeros((step, 1), f32)
            for b in range(fs):
                v = read(b, r).astype(f32)
                total = total + jnp.sum(v * v, axis=-1, keepdims=True)
            scale = lax.rsqrt(total / (fs * c) + EPS)
            for b in range(fs):
                v = read(b, r).astype(f32)
                nrm[s, b, r, :] = (v * scale * gain[:, b * c : (b + 1) * c]).astype(bf16)
            return 0

        lax.fori_loop(0, length // step, body, 0)

    def tok_block(s):
        return lambda b, r: tok[s, b // hb, r, b % hb * c : (b % hb + 1) * c]

    @scoped("dot")
    def dot(b, s, at, first):
        n = buf[b].shape[2]
        tile = 256
        src = pl.ds(at * ny, ny)
        rows = jnp.concatenate([nrm[s, at * ny + i] for i in range(ny)], axis=1)

        def one(cols):
            v = jnp.dot(
                rows, buf[b][src, :, cols].reshape(ny * c, -1), preferred_element_type=f32
            )
            if first:
                acc[s, :, cols] = v
            else:
                acc[s, :, cols] += v

        def body(i, _):
            one(pl.ds(pl.multiple_of(i * tile, tile), tile))
            return 0

        lax.fori_loop(0, n // tile, body, 0)
        if n % tile:
            one(pl.ds(n // tile * tile, n % tile))

    def from_twin(b, d, sub=0):
        for g, group in enumerate(groups):
            if group[0] == b:
                arrived(over(g, d, 1))

    def ready(b, i):
        need(b, i + 1)
        if i >= 0:
            from_twin(b, lax.rem(z - nth(i) + nz, nz))

    def dots(b, s, i):
        run(DOT[b], dot, b, s, z if i < 0 else nth(i), i < 0)

    @scoped("recur")
    def recurrence(s, lo, hi):
        extra = jnp.transpose(ex[s])[:, :1]

        def body(i, _):
            lanes = pl.ds(pl.multiple_of(i * LANES, LANES), LANES)
            glanes = pl.ds(pl.multiple_of(width + i * LANES, LANES), LANES)
            wide = pl.ds(pl.multiple_of(y * width + i * LANES, LANES), LANES)
            values = (acc[s, :, lanes] * iscale_ref[:, wide]).astype(bf16).astype(f32)
            gate = (acc[s, :, glanes] * gscale_ref[:, wide]).astype(bf16).astype(f32)
            gated[s, :, lanes] = rec_block(
                values, gate, taps_ref[:, wide], maps[i], rates[:, lanes], extra
            )
            return 0

        lax.fori_loop(lo, hi, body, 0)

    def part_of(j, i):
        return pl.ds(j * subs, subs) if i is None else pl.ds(j * subs + i, 1)

    def tp_copy(l, s, j, i=None):
        at, sem = part_of(j, i), j * subs + (i or 0)
        return copy(thr_s.at[s, at], thr_r.at[s, at], ps.at[l, s, sem], pr.at[l, s, sem], over_tp)

    def x_copy(l, s, j, i=None):
        at, sem = part_of(j, i), j * subs + (i or 0)
        return copy(
            thr_s.at[s, at], xr.at[1 - s, at], xss.at[l, s, sem], xrs.at[l, 1 - s, sem], pair
        )

    def x_arrived(l, s, j, i=None):
        x_copy(l, 1 - s, j, i).wait_recv()

    @scoped("project")
    def project(l, s, j, i=None):
        theirs, mine = (1 - tp) * hb + j, tp * hb + j

        def product(at):
            acts, w = (gated, b1.at[at]) if l == 0 else (hid, b3.at[at])
            return jnp.dot(acts[s], w[...], preferred_element_type=f32)

        def put(to, v):
            for k in range(subs) if i is None else (i,):
                cols = slice(k * cs, (k + 1) * cs) if i is None else slice(0, cs)
                to[s, j * subs + k] = v[:, cols].astype(to.dtype)

        put(thr_s, product(theirs))
        tp_copy(l, s, j, i).start()
        put(part, product(mine))

    @scoped("send")
    def send(l, s, j, i=None):
        tp_copy(l, s, j, i).wait()
        at = part_of(j, i)
        total = part[s, at] + thr_r[s, at].astype(f32)
        thr_s[s, at] = total.astype(bf16)
        x_copy(l, s, j, i).start()
        if l == 0:
            part[s, at] = total

    def residual(scale, s, j, k):
        at = j * subs + k
        total = part[s, at] + xr[s, at].astype(f32)
        if scale is dscale_ref:
            total = total + thr_r[s, at].astype(f32)
        lo = j * c + k * cs
        cols = slice(lo, lo + cs)
        factor = jnp.where(
            tp == 0, scale[:, cols], scale[:, columns + lo : columns + lo + cs]
        )
        tok[s, tp, :, cols] = (tok[s, tp, :, cols].astype(f32) + total * factor).astype(bf16)

    chunk = max(c, LANES)
    chunks = columns // chunk

    def m_tp(s, q):
        at = tok.at[s, tp, :, pl.ds(q * chunk, chunk)]
        return copy(at, at, ms.at[s, q], mr.at[s, q], over_tp)

    @scoped("mixed")
    def mixed(s, q):
        for j in range(q * chunk // c, (q + 1) * chunk // c):
            x_arrived(0, s, j)
            for k in range(subs):
                residual(oscale_ref, s, j, k)
        m_tp(s, q).start()

    @scoped("hide")
    def hide(s):
        def silu_up(g, u):
            return (g / (1.0 + jnp.exp(-g)) * u).astype(bf16)

        def body(i, _):
            step = 128
            r = pl.ds(pl.multiple_of(i * step, step), step)
            for k in range(0, main, LANES):
                m = main + k
                g = acc[s, r, k : k + LANES] * guscale[0:1, k : k + LANES]
                u = acc[s, r, m : m + LANES] * guscale[0:1, m : m + LANES]
                hid[s, r, k : k + LANES] = silu_up(g, u)
            if rest:
                both = acc[s, r, 2 * main :] * guscale[0:1, 2 * main :]
                hid[s, r, main:] = silu_up(both, pltpu.roll(both, rest, 1))[:, :rest]
            return 0

        lax.fori_loop(0, length // 128, body, 0)

    def store(q):
        cols = pl.ds(q * chunk, chunk)
        return pltpu.make_async_copy(tok.at[0, tp, :, cols], o_ref.at[:, cols], lsem.at[q])

    @scoped("finish")
    def finish(q):
        m_tp(0, q).wait_send()
        for j in range(q * chunk // c, (q + 1) * chunk // c):
            for k in range(subs):
                tp_copy(1, 0, j, k).wait_recv()
                x_arrived(1, 0, j, k)
                residual(dscale_ref, 0, j, k)
        store(q).start()

    ranks = range(-1, nz - 1)
    blocks = width // LANES
    spans = [(lo, min(lo + 2, blocks)) for lo in range(0, blocks, 2)]
    wait_until(6.0, arrived, tok_tp)
    run(1.3, norm, tok_block(0), 0, mgain_ref)
    next_slot()
    tok_x.start()
    run(1.4, pack)
    run(1.0, tables)
    wait_until(TOKENS, arrived, tok_x)
    tok_xtp.start()
    own_y(3)
    own_y(4)
    wait_until(TOKENS + 3.0, arrived, tok_xtp)
    run(1.3, norm, tok_block(1), 1, mgain_ref)
    for sent in (tok_tp, tok_x, tok_xtp, extra_x):
        sent.wait_send()
    clock[0] = max(clock[0], TOKENS + 6.0)
    for i in ranks:
        ready(0, i)
        dots(0, 1, i)
    arrived(extra_x)
    for s in (1, 0):
        for span in spans:
            run(3.3, recurrence, s, *span)
        if s:
            for i in ranks:
                dots(0, 0, i)
            for i in ranks:
                ready(1, i)
        for j in range(hb):
            run(0.9, project, 0, s, j)
            if j:
                run(0.4, send, 0, s, j - 1)
        run(0.4, send, 0, s, hb - 1)
    start = clock[0] - 8
    for s in (0, 1):
        for q in range(chunks):
            wait_until(start + HOP * (s + (q + 1) / chunks), mixed, s, q)
        if s == 0:
            pl.semaphore_signal(free, inc=1, device_id=pair, device_id_type=MESH)
        else:
            ready(2, -1)
            dots(2, 0, -1)
        for q in range(chunks):
            arrived(m_tp(s, q))
        run(1.3, norm, tok_block(s), s, fgain_ref)
    dots(2, 1, -1)
    for i in ranks[1:]:
        ready(2, i)
        dots(2, 1, i)
    run(0.8, hide, 1)
    for j in range(hb):
        for s in range(2):
            x_copy(0, s, j).wait_send()
    pl.semaphore_wait(free, 1)

    def blocks_of(i):
        for w in (0, 1):
            for k in range(half):
                yield w, k, lax.rem(z - k + nz, half) * ny + (1 - rep if w else rep)

    def others():
        for i in ranks[1:]:
            dots(2, 0, i)
        hide(0)

    g = len(groups) - 1
    for w, k, j in blocks_of(0):
        d = half if k == 0 and w == 0 else nz - 1
        if (w, k) == (1, 0):
            others()
        while slots and slots[0] <= (g, d):
            next_slot()
        if w:
            if k:
                from_twin(3, k)
            from_twin(3, k + half)
        project(1, 1, j)
        send(1, 1, j)
    for w, k, j in blocks_of(0):
        project(1, 0, j)
    @scoped("passed")
    def passed():
        for g in range(len(groups)):
            for k in range(1, nz):

                @pl.when(can_up(k))
                def _():
                    up(g, k, z - k + 1).wait_send()

                @pl.when(can_down(k))
                def _():
                    down_z(g, k, z + k - 1).wait_send()

                over(g, k).wait_send()
            swap(g).wait_send()

    passed()
    for q in range(chunks):
        finish(q)

    @scoped("sent")
    def sent_all():
        for j in range(hb):
            for i in range(subs):
                x_copy(1, 1, j, i).wait_send()
                tp_copy(1, 0, j, i).wait_send()
        for q in range(chunks):
            m_tp(1, q).wait_send()

    @scoped("stored")
    def stored():
        for q in range(chunks):
            store(q).wait()

    sent_all()
    stored()


def layer(ny, nz, tokens, lru_input, lru_gate, lru_output, ffn_gate, ffn_up, ffn_down, *rest):
    fs = ny * nz
    length, columns = tokens.shape
    c = lru_input.shape[0]
    hb = columns // c
    width, hidden = lru_output.shape[0] // 2, ffn_down.shape[0] // 2
    subs = 1
    cut = (hb * subs, length, c // subs)
    bf16, f32 = jnp.bfloat16, jnp.float32
    dma = pltpu.SemaphoreType.DMA
    vmem = pl.BlockSpec(memory_space=pltpu.VMEM)
    hbm = pl.BlockSpec(memory_space=pl.ANY)
    return pl.pallas_call(
        functools.partial(layer_kernel, ny, nz),
        out_shape=jax.ShapeDtypeStruct((length, columns), bf16),
        in_specs=[hbm] * 7 + [vmem] * len(rest),
        out_specs=hbm,
        scratch_shapes=[
            pltpu.VMEM((2, 2, length, columns), bf16),
            pltpu.VMEM((2, 8, length), f32),
            pltpu.VMEM((2, fs, length, c), bf16),
            pltpu.VMEM((fs, c, 2 * width), bf16),
            pltpu.VMEM((fs, width, c), bf16),
            pltpu.VMEM((fs, c, 2 * hidden), bf16),
            pltpu.VMEM((fs, hidden, c), bf16),
            pltpu.VMEM((c, 2 * width), bf16),
            pltpu.VMEM((width, c), bf16),
            pltpu.VMEM((c, 2 * hidden), bf16),
            pltpu.VMEM((hidden, c), bf16),
            pltpu.VMEM((2, length, 2 * max(width, hidden)), f32),
            pltpu.VMEM((2, length, width), bf16),
            pltpu.VMEM((2, length, hidden), bf16),
            pltpu.VMEM((2, *cut), f32),
            pltpu.VMEM((2, *cut), bf16),
            pltpu.VMEM((2, *cut), bf16),
            pltpu.VMEM((2, *cut), bf16),
            pltpu.VMEM((width // LANES, LANES, 2 * LANES), f32),
            pltpu.VMEM((1, width), f32),
            pltpu.VMEM((8, 2 * hidden), f32),
            dma((max(32, columns // LANES),)),
            dma((10, nz)),
            dma((10, nz)),
            dma((10, nz)),
            dma((10, nz)),
            dma((10, nz)),
            dma((10, nz)),
            dma((4,)),
            dma((4,)),
            dma((2, 2, cut[0])),
            dma((2, 2, cut[0])),
            dma((2, 2, cut[0])),
            dma((2, 2, cut[0])),
            dma((2, hb)),
            dma((2, hb)),
            pltpu.SemaphoreType.REGULAR,
        ],
        compiler_params=pltpu.CompilerParams(
            collective_id=0, has_side_effects=True, vmem_limit_bytes=67_000_000
        ),
        name="layer",
    )(tokens, lru_input, lru_gate, lru_output, ffn_gate, ffn_up, ffn_down, *rest)


def local(mesh_fs, *args):
    (
        tokens,
        mix_gain,
        lru_input,
        lru_gate,
        lru_input_scale,
        lru_gate_scale,
        conv_weight,
        recur_gate,
        input_gate,
        decay_rate,
        extra_decay,
        lru_output,
        lru_output_scale,
        ffn_gain,
        ffn_gate,
        ffn_up,
        ffn_gate_scale,
        ffn_up_scale,
        ffn_down,
        ffn_down_scale,
    ) = args
    ny = 2 if mesh_fs % 2 == 0 else 1
    return layer(
        ny,
        mesh_fs // ny,
        tokens,
        lru_input,
        lru_gate,
        lru_output,
        ffn_gate,
        ffn_up,
        ffn_down,
        extra_decay[None, :],
        mix_gain[None, :],
        ffn_gain[None, :],
        lru_input_scale[None, :],
        lru_gate_scale[None, :],
        lru_output_scale[None, :],
        jnp.stack([ffn_gate_scale, ffn_up_scale]),
        ffn_down_scale[None, :],
        conv_weight,
        recur_gate,
        input_gate,
        decay_rate[None, :],
    )


def solution(mesh):
    in_specs = (
        P(("rep", "fs"), "tp"),
        P(),
        P("fs", "tp"),
        P("fs", "tp"),
        P("tp"),
        P("tp"),
        P(None, "tp"),
        P("tp", None, None),
        P("tp", None, None),
        P("tp"),
        P(("rep", "fs")),
        P("tp", "fs"),
        P(),
        P(),
        P("fs", "tp"),
        P("fs", "tp"),
        P("tp"),
        P("tp"),
        P("tp", "fs"),
        P(),
    )
    out_specs = P(("rep", "fs"), "tp")
    mesh_fs = mesh.shape["fs"]
    return jax.shard_map(
        lambda *args: local(mesh_fs, *args),
        mesh=mesh,
        in_specs=in_specs,
        out_specs=out_specs,
        check_vma=False,
    )
```
